32 devices in a mesh: gr: 2 (over x), sp: 4 (over z), tp: 4 (over y, core).
Axes of the slice: x: 2, y: 2, z: 4, core: 2. Of those that a mesh axis runs over, the one named last changes fastest.
Arguments:
- tokens: bfloat16 [8, 8192, 2048], P('gr', ('sp', 'tp')), parts along dimension 0, may hold values from -6 to 6
- norm_gain: float32 [2048], replicated, may hold values from 0.1 to 1.9
- w_key: bfloat16 [2048, 256], replicated, may hold values from -0.125 to 0.125
- w_value: bfloat16 [2048, 256], replicated, may hold values from -0.125 to 0.125
- new_query: bfloat16 [8, 32, 64], P('gr'), parts along dimension 0, may hold values from -360 to 360
- cum_gate: float32 [8, 4, 8192], P(('gr', 'sp'), 'tp'), parts along dimension 0, may hold values from -1025 to 0, as said below
Outputs:
- kv_cache: bfloat16 [8, 4, 8192, 128], P(('gr', 'sp'), 'tp'), parts along dimension 0
- first_read: float32 [8, 32, 64], P('gr'), parts along dimension 0
The draws below stay inside these ranges and needn't reach their ends.
There are 2 independent parts, one for each index of `gr`. The reference program is written for one: setup_inputs(seed, part) draws one part's arguments, and reference() takes and returns one part's arrays. A program takes and returns all parts, laid end to end along the dimension named above; an argument that names none is the same for every part. Nothing has to cross between parts.
Inputs may be any that keep to these rules, and one draw needn't show every extreme that they name: `cum_gate`: for each sequence and key head, the running sum along the positions of the sequence of negative log forget gates; it never rises from one position to the next.
All inputs are finite; a program needn't handle non-finite values.
Results may differ from the reference program's by a relative error of at most 0.0014.
The reference program's roundings to bfloat16 on the way (of `normed`, `keys_all` and `values_all`) count: a program that leaves them out, or rounds other values in their place, can miss the bound.
Values may be sent and summed in bfloat16 or wider, within the bound.
A program may use at most 64 MiB of HBM per device.

```python
from functools import partial
import jax
import jax.numpy as jnp
from jax import lax

D = 2048
HD = 64
QH = 32
KVH = 4
SEQS = 4
POS_DEV = 512
BLOCKS = 16
LEN = 8192
CLASSES = 1
HALVES = 1
PIECE = 512


def draw_new_query(key, part):
    base = 3.0 * jax.random.normal(jax.random.fold_in(key, 3), (SEQS, QH, HD), jnp.float32)
    base = jnp.clip(base, -18.0, 18.0)
    return base.astype(jnp.bfloat16)


def draw_cum_gate(key, part):
    flag_key = jax.random.fold_in(key, 11)
    fast_flags = jax.random.randint(flag_key, (SEQS, KVH, 1, 1), 0, 2) == 1
    fast_rate = jnp.exp(jax.random.uniform(jax.random.fold_in(key, 12), (SEQS, KVH, 1, 1), jnp.float32, jnp.log(0.01), jnp.log(1.0 / 30.0)))
    slow_rate = jnp.exp(jax.random.uniform(jax.random.fold_in(key, 13), (SEQS, KVH, 1, 1), jnp.float32, jnp.log(0.3), jnp.log(1.0))) / LEN
    base_rate = jnp.where(fast_flags, fast_rate, slow_rate)
    block_factor = jnp.exp(jax.random.uniform(jax.random.fold_in(key, 14), (SEQS, KVH, BLOCKS, 1), jnp.float32, jnp.log(0.5), jnp.log(2.0)))
    jitter = jax.random.uniform(jax.random.fold_in(key, 15), (SEQS, KVH, BLOCKS, POS_DEV), jnp.float32, 0.25, 1.75)
    log_gate = -(base_rate * block_factor * jitter)
    running = jnp.cumsum(log_gate.reshape(SEQS, KVH, LEN), axis=-1)
    laid = running.reshape(SEQS, KVH, BLOCKS, CLASSES, HALVES, PIECE).transpose(0, 3, 1, 4, 2, 5)
    return laid.reshape(SEQS * CLASSES, KVH * HALVES, BLOCKS * PIECE)


def block_levels(key, dims, cuts, least, high):
    loudness = 1.0
    for dim, parts in cuts:
        heights = jax.random.uniform(jax.random.fold_in(jax.random.fold_in(key, 6), dim), (parts,), jnp.float32, least / len(cuts), high / len(cuts))
        loudness = loudness * jnp.repeat(jnp.exp(heights), dims[dim] // parts).reshape((-1,) + (1,) * (len(dims) - 1 - dim))
    return loudness


def bell_draw(rng, shape, deviation, reach, split=(), kind=jnp.bfloat16):
    factor_of = block_levels(rng, shape, split, -0.22, 0.18) if split else 1.0
    values = jax.random.normal(rng, shape, jnp.float32) * deviation * factor_of
    return jnp.minimum(jnp.maximum(values, -reach), reach).astype(kind)


def setup_inputs(seed: int = 0, part: int = 0) -> dict:
    key_of = jax.random.split(jax.random.key(seed), 7)
    part_splits = jax.random.split(jax.random.fold_in(key_of[6], part), 7)
    return {
        "tokens": bell_draw(part_splits[0], (SEQS, LEN, D), 1.0, 6.0, ((1, 16),)),
        "norm_gain": jnp.clip(1.0 + 0.18 * jax.random.normal(key_of[1], (D,), jnp.float32), 0.1, 1.9),
        "w_key": bell_draw(key_of[2], (D, KVH * HD), D ** -0.5, 0.125),
        "w_value": bell_draw(key_of[3], (D, KVH * HD), D ** -0.5, 0.125),
        "new_query": draw_new_query(jax.random.fold_in(jax.random.fold_in(key_of[6], part), 71), part),
        "cum_gate": draw_cum_gate(jax.random.fold_in(jax.random.fold_in(key_of[6], part), 71), part),
    }


NORM_FLOOR = 0.05

def project_block(norm_gain, w_key, w_value, pos_block):
    widened = pos_block.astype(jnp.float32)
    inverse_rms = lax.rsqrt(lax.optimization_barrier(jnp.mean(widened * widened, axis=-1, keepdims=True)) + NORM_FLOOR)
    normed = (widened * inverse_rms * norm_gain.astype(jnp.float32)).astype(jnp.bfloat16)
    keys_made = jnp.dot(normed, w_key, preferred_element_type=jnp.float32).astype(jnp.bfloat16)
    values_made = jnp.dot(normed, w_value, preferred_element_type=jnp.float32).astype(jnp.bfloat16)
    keys_made = keys_made.reshape(POS_DEV, KVH, HD)
    values_made = values_made.reshape(POS_DEV, KVH, HD)
    return jnp.concatenate([keys_made, values_made], axis=-1)

def reference(tokens, norm_gain, w_key, w_value, new_query, cum_gate):
    pos_blocks = tokens.reshape(SEQS * BLOCKS, POS_DEV, D)
    stacked = lax.map(partial(project_block, norm_gain, w_key, w_value), pos_blocks)
    stacked = stacked.reshape(SEQS, BLOCKS, CLASSES, HALVES, PIECE, KVH, 2 * HD)
    kv_cache = stacked.transpose(0, 2, 5, 3, 1, 4, 6).reshape(SEQS * CLASSES, KVH * HALVES, BLOCKS * PIECE, 2 * HD)
    per_head = kv_cache.reshape(SEQS, CLASSES, KVH, HALVES, BLOCKS * PIECE, 2 * HD)
    per_head = per_head.transpose(0, 2, 1, 3, 4, 5).reshape(SEQS, KVH, LEN, 2 * HD)
    gates = cum_gate.reshape(SEQS, CLASSES, KVH, HALVES, BLOCKS * PIECE)
    gates = gates.transpose(0, 2, 1, 3, 4).reshape(SEQS, KVH, LEN)
    keys_all = per_head[..., :HD].astype(jnp.float32)
    values_all = per_head[..., HD:].astype(jnp.float32)
    grouped = new_query.astype(jnp.float32).reshape(SEQS, KVH, QH // KVH, HD)
    scores = jnp.einsum('sgqd,sgpd->sgqp', grouped, keys_all, precision=lax.Precision.HIGHEST)
    scores = scores * HD ** (-0.5) - gates[:, :, None, :]
    row_top = lax.optimization_barrier(jnp.max(scores, axis=-1, keepdims=True))
    weights = jnp.exp(scores - row_top)
    row_total = lax.optimization_barrier(jnp.sum(weights, axis=-1))
    summed = jnp.einsum('sgqp,sgpd->sgqd', weights, values_all, precision=lax.Precision.HIGHEST)
    first_read = (summed / row_total[..., None]).reshape(SEQS, QH, HD)
    return (kv_cache, first_read)
```

```python
import functools

import jax
import jax.numpy as jnp
from jax import lax
from jax.experimental import pallas as pl
from jax.experimental.pallas import tpu as pltpu
from jax.sharding import PartitionSpec as P

HD = 64
NORM_FLOOR = 0.05
SCORE_FLOOR = -1e30
MESH = pl.DeviceIdType.MESH
TILE = 256
CHUNKS = 4
NORM_ROWS = 16
VMEM_BYTES = 60_000_000


def sequence_at(step, own, count):
    low = own < count // 2
    first = jnp.where(low, count - 1 - step, step)
    following = jnp.where(low, count - 2 - step, step + 1)
    own_step = jnp.where(low, count - 1 - own, own)
    shifted = jnp.where(step >= own_step, following, first)
    return jnp.where(step == count - 1, own, shifted)


def kernel(
    sizes,
    tokens_hbm,
    gain_hbm,
    wk_hbm,
    wv_hbm,
    query_hbm,
    gate_hbm,
    cache_ref,
    read_ref,
    tok_buf,
    wk_buf,
    wv_buf,
    gain_ref,
    query_ref,
    gate_ref,
    norm_buf,
    staging,
    gates_in,
    own_parts,
    parts_in,
    partials,
    tok_sem,
    w_sem,
    send_sem,
    recv_sem,
    part_send_sem,
    part_recv_sem,
    gate_send_sem,
    gate_recv_sem,
    early_send_sem,
    early_recv_sem,
    own_sem,
):
    sp_count, tp_count, seqs, heads, positions, width = sizes
    devices = sp_count * tp_count
    classes, halves = sp_count // seqs, tp_count // heads
    piece = positions // (classes * halves)
    sp, tp = lax.axis_index("sp"), lax.axis_index("tp")
    me = sp * tp_count + tp
    seq_me, head_me = sp // classes, tp // halves
    tile = min(TILE, positions)
    tiles = positions // tile
    sub = min(piece, tile)

    def token_copy(step, part):
        seq = sequence_at(step, seq_me, seqs)
        rows = pl.ds(part * tile, tile)
        return pltpu.make_async_copy(
            tokens_hbm.at[seq, rows, :], tok_buf.at[step, rows, :], tok_sem.at[step, part]
        )

    k_copy = pltpu.make_async_copy(wk_hbm, wk_buf, w_sem.at[0])
    v_copy = pltpu.make_async_copy(wv_hbm, wv_buf, w_sem.at[1])
    gain_copy = pltpu.make_async_copy(gain_hbm, gain_ref, w_sem.at[2])
    query_copy = pltpu.make_async_copy(query_hbm, query_ref, w_sem.at[3])
    gate_copy = pltpu.make_async_copy(gate_hbm, gate_ref, w_sem.at[4])
    gain_copy.start()
    gate_copy.start()
    query_copy.start()
    token_copy(0, 0).start()
    k_copy.start()
    v_copy.start()
    for step in range(seqs):
        for part in range(tiles):
            if step or part:
                token_copy(step, part).start()
    gain_copy.wait()

    barrier = pltpu.get_barrier_semaphore()

    def greet(other, carry):
        @pl.when(other != me)
        def _():
            pl.semaphore_signal(
                barrier,
                inc=1,
                device_id={"sp": other // tp_count, "tp": other % tp_count},
                device_id_type=MESH,
            )

        return carry

    lax.fori_loop(0, devices, greet, 0)

    def project(index, carry):
        step, part = index // tiles, index % tiles
        seq = sequence_at(step, seq_me, seqs)
        row0 = pl.multiple_of(part * tile, tile)
        token_copy(step, part).wait()
        gain = gain_ref[...]
        for piece_row in range(0, tile, NORM_ROWS):
            block = tok_buf[step, pl.ds(row0 + piece_row, NORM_ROWS), :].astype(jnp.float32)
            mean = jnp.mean(block * block, axis=-1, keepdims=True)
            normed = block * lax.rsqrt(mean + NORM_FLOOR) * gain
            norm_buf[pl.ds(piece_row, NORM_ROWS), :] = normed.astype(jnp.bfloat16)

        @pl.when(index == 0)
        def _():
            k_copy.wait()
            v_copy.wait()

        normed_tile = norm_buf[...]
        keys = jnp.dot(normed_tile, wk_buf[...], preferred_element_type=jnp.float32)
        values = jnp.dot(normed_tile, wv_buf[...], preferred_element_type=jnp.float32)
        keys = keys.astype(jnp.bfloat16)
        values = values.astype(jnp.bfloat16)
        for head in range(heads):
            cols = slice(head * HD, (head + 1) * HD)
            both = jnp.concatenate([keys[:, cols], values[:, cols]], axis=1)
            staging[seq * heads + head, pl.ds(row0, tile), :] = both

        @pl.when(index == 0)
        def _():
            pl.semaphore_wait(barrier, devices - 1)
            gate_copy.wait()
            for_others(send_gate)

        @pl.when(step == 0)
        def _():
            send_tile(index)

        return carry

    window = max(piece, 128)

    def for_others(body):
        def visit(other, carry):
            @pl.when(other != me)
            def _():
                body(other)

            return carry

        lax.fori_loop(0, devices, visit, 0)

    def place(other):
        return {"sp": other // tp_count, "tp": other % tp_count}

    def gate_window(other):
        start = pl.multiple_of(other * piece // window * window, window)
        return gate_ref.at[:, pl.ds(start, window)]

    def send_gate(other):
        pltpu.make_async_remote_copy(
            src_ref=gate_window(other),
            dst_ref=gates_in.at[me],
            send_sem=gate_send_sem,
            recv_sem=gate_recv_sem,
            device_id=place(other),
            device_id_type=MESH,
        ).start()

    def send_tile(index):
        step, part = index // tiles, index % tiles
        seq = sequence_at(step, seq_me, seqs)
        row0 = part * tile
        for head in range(heads):
            for piece_row in range(0, tile, sub):
                row = pl.multiple_of(row0 + piece_row, sub)
                slot = row // piece
                to_sp = seq * classes + slot // halves
                to_tp = head * halves + slot % halves
                dest = to_sp * tp_count + to_tp
                landing = pl.multiple_of(me * piece + row % piece, sub)
                source = staging.at[seq * heads + head, pl.ds(row, sub), :]
                target = cache_ref.at[pl.ds(landing, sub), :]

                @pl.when(dest != me)
                def _():
                    pltpu.make_async_remote_copy(
                        src_ref=source,
                        dst_ref=target,
                        send_sem=send_sem,
                        recv_sem=recv_sem,
                        device_id={"sp": to_sp, "tp": to_tp},
                        device_id_type=MESH,
                    ).start()

                @pl.when(dest == me)
                def _():
                    pltpu.make_async_copy(source, target, own_sem).start()

    def send_tiles(first, last):
        def visit(index, carry):
            send_tile(index)
            return carry

        lax.fori_loop(first, last, visit, 0)

    def wait_bytes(ref, sem):
        pltpu.make_async_copy(ref, ref, sem).wait()

    lax.fori_loop(0, seqs * tiles, project, 0)

    query_copy.wait()
    group = query_ref.shape[2]
    others = parts_in.at[pl.ds(0, devices - 1)]
    gates_in[me] = gate_ref[:, pl.ds(pl.multiple_of(me * piece // window * window, window), window)]
    other_gates = gates_in.at[pl.ds(0, devices - 1)]
    wait_bytes(other_gates, gate_recv_sem)
    lane = lax.broadcasted_iota(jnp.int32, (group, 2 * HD), 1)
    line = lax.broadcasted_iota(jnp.int32, (group, 2 * HD), 0)
    half = group // 2

    def pack(ref, slot, top, total, out):
        folded = jnp.concatenate([out[:half], out[half:]], axis=1)
        stats = jnp.where(lane == line, top, 0.0) + jnp.where(lane == line + group, total, 0.0)
        for k in range(half):
            ref[slot, :, k * 2 * HD : (k + 1) * 2 * HD] = folded[k : k + 1]
        ref[slot, :, half * 2 * HD :] = jnp.sum(stats, axis=0, keepdims=True)

    def unpack(ref, slot):
        rows = [ref[slot, :, k * 2 * HD : (k + 1) * 2 * HD] for k in range(half + 1)]
        out = jnp.concatenate([r[:, :HD] for r in rows[:half]] + [r[:, HD:] for r in rows[:half]])
        top = jnp.sum(jnp.where(lane == line, rows[half], 0.0), axis=1, keepdims=True)
        total = jnp.sum(jnp.where(lane == line + group, rows[half], 0.0), axis=1, keepdims=True)
        return top, total, out

    def merge(left, right):
        best = jnp.maximum(left[0], right[0])
        scale_left, scale_right = jnp.exp(left[0] - best), jnp.exp(right[0] - best)
        total = left[1] * scale_left + right[1] * scale_right
        return best, total, left[2] * scale_left + right[2] * scale_right

    def attend(seq, carry):
        for head in range(heads):
            query = query_ref[seq, head]
            query = jnp.concatenate([query, jnp.zeros_like(query)], axis=1)
            for slot in range(classes * halves):
                dest = (seq * classes + slot // halves) * tp_count + head * halves + slot % halves
                block = staging[seq * heads + head, slot * piece : (slot + 1) * piece, :]
                gates = gates_in[dest]
                choices = [gates[:, k * piece : (k + 1) * piece] for k in range(window // piece)]
                gate = choices[0]
                for k in range(1, len(choices)):
                    gate = jnp.where(me % (window // piece) == k, choices[k], gate)
                scores = lax.dot_general(
                    query, block, (((1,), (1,)), ((), ())), preferred_element_type=jnp.float32
                )
                scores = scores * HD ** (-0.5) - gate
                top = jnp.max(scores, axis=1, keepdims=True)
                weights = jnp.exp(scores - top)
                total = jnp.sum(weights, axis=1, keepdims=True)
                first = weights.astype(jnp.bfloat16)
                rest = weights - first.astype(jnp.float32)
                second = rest.astype(jnp.bfloat16)
                third = (rest - second.astype(jnp.float32)).astype(jnp.bfloat16)
                summed = jnp.dot(first, block, preferred_element_type=jnp.float32)
                summed += jnp.dot(second, block, preferred_element_type=jnp.float32)
                summed += jnp.dot(third, block, preferred_element_type=jnp.float32)
                pack(own_parts, dest, top, total, summed[:, HD:])
        return carry

    lax.fori_loop(0, seqs, attend, 0)
    parts_in[me] = own_parts[me]

    def send_part(other):
        pltpu.make_async_remote_copy(
            src_ref=own_parts.at[other],
            dst_ref=parts_in.at[me],
            send_sem=early_send_sem,
            recv_sem=early_recv_sem,
            device_id=place(other),
            device_id_type=MESH,
        ).start()

    for_others(send_part)
    held = tiles + max(tiles // 2, 1)
    send_tiles(2 * tiles, seqs * tiles)
    send_tiles(tiles, held)

    wait_bytes(others, early_recv_sem)
    merged = lax.fori_loop(
        1, devices, lambda n, held_sum: merge(held_sum, unpack(parts_in, n)), unpack(parts_in, 0)
    )
    pack(partials, me, *merged)

    def send_read(other):
        pltpu.make_async_remote_copy(
            src_ref=partials.at[me],
            dst_ref=partials.at[me],
            send_sem=part_send_sem,
            recv_sem=part_recv_sem,
            device_id=place(other),
            device_id_type=MESH,
        ).start()

    for_others(send_read)
    send_tiles(held, 2 * tiles)

    wait_bytes(partials.at[pl.ds(0, devices - 1)], part_recv_sem)
    for seq in range(seqs):
        for head in range(heads):
            slots = [
                unpack(partials, (seq * classes + c) * tp_count + head * halves + b)
                for c in range(classes)
                for b in range(halves)
            ]
            _, total, out = functools.reduce(merge, slots)
            read_ref[seq, pl.ds(head * group, group), :] = out / total
    wait_bytes(other_gates, gate_send_sem)
    wait_bytes(others, early_send_sem)
    wait_bytes(others, part_send_sem)
    wait_bytes(cache_ref.at[pl.ds(0, piece), :], own_sem)
    sent = cache_ref.at[pl.ds(0, (devices - 1) * piece), :]
    wait_bytes(sent, send_sem)
    wait_bytes(sent, recv_sem)


def settle(cache_in, read_in, cache_out, read_out, sems):
    copies = [
        pltpu.make_async_copy(cache_in, cache_out, sems.at[0]),
        pltpu.make_async_copy(read_in, read_out, sems.at[1]),
    ]
    for copy in copies:
        copy.start()
    for copy in copies:
        copy.wait()


def solution(mesh):
    sp_count, tp_count = mesh.shape["sp"], mesh.shape["tp"]
    devices = sp_count * tp_count

    def shards(tokens, norm_gain, w_key, w_value, new_query, cum_gate):
        seqs, positions, width = tokens.shape
        heads = w_key.shape[1] // HD
        columns = w_key.shape[1]
        query_heads = new_query.shape[1]
        group = query_heads // heads
        length = cum_gate.shape[-1]
        tile = min(TILE, positions)
        sizes = (sp_count, tp_count, seqs, heads, positions, width)
        vmem = pl.BlockSpec(memory_space=pltpu.VMEM)
        anywhere = pl.BlockSpec(memory_space=pltpu.HBM)
        cache, first_read = pl.pallas_call(
            functools.partial(kernel, sizes),
            out_shape=(
                pltpu.VMEM((length, 2 * HD), jnp.bfloat16),
                pltpu.VMEM((seqs, query_heads, HD), jnp.float32),
            ),
            in_specs=[anywhere] * 6,
            out_specs=(vmem, vmem),
            scratch_shapes=[
                pltpu.VMEM((seqs, positions, width), jnp.bfloat16),
                pltpu.VMEM((width, columns), jnp.bfloat16),
                pltpu.VMEM((width, columns), jnp.bfloat16),
                pltpu.VMEM((1, width), jnp.float32),
                pltpu.VMEM((seqs, heads, group, HD), jnp.bfloat16),
                pltpu.VMEM((1, length), jnp.float32),
                pltpu.VMEM((tile, width), jnp.bfloat16),
                pltpu.VMEM((seqs * heads, positions, 2 * HD), jnp.bfloat16),
                pltpu.VMEM((devices, 1, max(length // devices, 128)), jnp.float32),
                pltpu.VMEM((devices, 1, (group // 2 + 1) * 2 * HD), jnp.float32),
                pltpu.VMEM((devices, 1, (group // 2 + 1) * 2 * HD), jnp.float32),
                pltpu.VMEM((devices, 1, (group // 2 + 1) * 2 * HD), jnp.float32),
                pltpu.SemaphoreType.DMA((seqs, positions // tile)),
                pltpu.SemaphoreType.DMA((5,)),
                *[pltpu.SemaphoreType.DMA] * 9,
            ],
            compiler_params=pltpu.CompilerParams(
                collective_id=0, has_side_effects=True, vmem_limit_bytes=VMEM_BYTES
            ),
        )(
            tokens,
            norm_gain.reshape(1, width),
            w_key,
            w_value,
            new_query.reshape(seqs, heads, group, HD),
            cum_gate.reshape(1, length),
        )
        cache, first_read = pl.pallas_call(
            settle,
            out_shape=(
                jax.ShapeDtypeStruct(cache.shape, cache.dtype),
                jax.ShapeDtypeStruct(first_read.shape, first_read.dtype),
            ),
            in_specs=[vmem] * 2,
            out_specs=(anywhere, anywhere),
            scratch_shapes=[pltpu.SemaphoreType.DMA((2,))],
            compiler_params=pltpu.CompilerParams(vmem_limit_bytes=VMEM_BYTES),
        )(
            pltpu.with_memory_space_constraint(cache, pltpu.VMEM),
            pltpu.with_memory_space_constraint(first_read, pltpu.VMEM),
        )
        return cache.reshape(1, 1, length, 2 * HD), first_read

    in_specs = (
        P("gr", ("sp", "tp"), None),
        P(),
        P(),
        P(),
        P("gr", None, None),
        P(("gr", "sp"), "tp", None),
    )
    out_specs = (P(("gr", "sp"), "tp", None, None), P("gr", None, None))
    return jax.shard_map(shards, mesh=mesh, in_specs=in_specs, out_specs=out_specs, check_vma=False)
```

```python
import functools

import jax
import jax.numpy as jnp
from jax import lax
from jax.experimental import pallas as pl
from jax.experimental.pallas import tpu as pltpu
from jax.sharding import PartitionSpec as P

HD = 64
NORM_FLOOR = 0.05
SCORE_FLOOR = -1e30
MESH = pl.DeviceIdType.MESH
TILE = 256
NORM_ROWS = 16
VMEM_BYTES = 60_000_000


def is_edge(own, count):
    return (own == 0) | (own == count - 1)


def sequence_at(step, own, count):
    low = own < count // 2
    moved = jnp.where(step == 0, count - 2, jnp.where(step <= count - 2, step - 1, step))
    turn = jnp.where(is_edge(own, count), moved, step)
    first = jnp.where(low, count - 1 - turn, turn)
    following = jnp.where(low, count - 2 - turn, turn + 1)
    own_step = jnp.where(low, count - 1 - own, own)
    shifted = jnp.where(turn >= own_step, following, first)
    return jnp.where(step == count - 1, own, shifted)


def kernel(
    sizes,
    tokens_hbm,
    gain_hbm,
    wk_hbm,
    wv_hbm,
    query_hbm,
    gate_hbm,
    cache_ref,
    read_ref,
    tok_buf,
    wk_buf,
    wv_buf,
    gain_ref,
    query_ref,
    gate_ref,
    norm_buf,
    staging,
    gates_in,
    own_parts,
    plane_parts,
    merged_parts,
    line_parts,
    finals,
    tok_sem,
    ramp_sem,
    w_sem,
    send_sem,
    recv_sem,
    gate_send_sem,
    gate_recv_sem,
    stage_send_sem,
    stage_recv_sem,
    own_sem,
):
    sp_count, tp_count, seqs, heads, positions, width = sizes
    devices = sp_count * tp_count
    classes, halves = sp_count // seqs, tp_count // heads
    piece = positions // (classes * halves)
    sp, tp = lax.axis_index("sp"), lax.axis_index("tp")
    me = sp * tp_count + tp
    seq_me, head_me = sp // classes, tp // halves
    tile = min(TILE, positions)
    tiles = positions // tile
    ramp = tile // 2
    window = max(piece, 128)
    edge = is_edge(seq_me, seqs)
    early = min(tiles + max(tiles // 2, 1), (seqs - 1) * tiles)
    last = (seqs - 1) * tiles

    def place(other):
        return {"sp": other // tp_count, "tp": other % tp_count}

    def for_others(body):
        def visit(other, carry):
            @pl.when(other != me)
            def _():
                body(other)

            return carry

        lax.fori_loop(0, devices, visit, 0)

    def for_line(body):
        def visit(other, carry):
            @pl.when(other != sp)
            def _():
                body(other)

            return carry

        lax.fori_loop(0, sp_count, visit, 0)

    def for_plane(body):
        def visit(other, carry):
            @pl.when(other != tp)
            def _():
                body(other)

            return carry

        lax.fori_loop(0, tp_count, visit, 0)

    def rows_copy(step, row0, rows, sem):
        seq = sequence_at(step, seq_me, seqs)
        part = pl.ds(row0, rows)
        return pltpu.make_async_copy(tokens_hbm.at[seq, part, :], tok_buf.at[step, part, :], sem)

    def ramp_copy(part):
        return rows_copy(0, part * ramp, ramp, ramp_sem.at[part])

    def token_copy(index):
        step, part = index // tiles, index % tiles
        row0 = pl.multiple_of(part * tile, tile)
        return rows_copy(step, row0, tile, tok_sem.at[step, part])

    k_copy = pltpu.make_async_copy(wk_hbm, wk_buf, w_sem.at[0])
    v_copy = pltpu.make_async_copy(wv_hbm, wv_buf, w_sem.at[1])
    gain_copy = pltpu.make_async_copy(gain_hbm, gain_ref, w_sem.at[2])
    query_copy = pltpu.make_async_copy(query_hbm, query_ref, w_sem.at[3])
    gate_copy = pltpu.make_async_copy(gate_hbm, gate_ref, w_sem.at[4])
    ramp_copy(0).start()
    gain_copy.start()
    k_copy.start()
    v_copy.start()
    ramp_copy(1).start()

    barrier = pltpu.get_barrier_semaphore()

    def greet(other):
        pl.semaphore_signal(barrier, inc=1, device_id=place(other), device_id_type=MESH)

    for_others(greet)
    gate_copy.start()
    query_copy.start()

    def normalize(step, row0, rows):
        gain = gain_ref[...]
        for piece_row in range(0, rows, NORM_ROWS):
            block = tok_buf[step, pl.ds(row0 + piece_row, NORM_ROWS), :].astype(jnp.float32)
            mean = jnp.mean(block * block, axis=-1, keepdims=True)
            normed = block * lax.rsqrt(mean + NORM_FLOOR) * gain
            norm_buf[pl.ds(piece_row, NORM_ROWS), :] = normed.astype(jnp.bfloat16)

    def multiply(step, row0, rows):
        seq = sequence_at(step, seq_me, seqs)
        normed_tile = norm_buf[:rows, :]
        keys = jnp.dot(normed_tile, wk_buf[...], preferred_element_type=jnp.float32)
        values = jnp.dot(normed_tile, wv_buf[...], preferred_element_type=jnp.float32)
        keys = keys.astype(jnp.bfloat16)
        values = values.astype(jnp.bfloat16)
        for head in range(heads):
            cols = slice(head * HD, (head + 1) * HD)
            both = jnp.concatenate([keys[:, cols], values[:, cols]], axis=1)
            staging[seq * heads + head, pl.ds(row0, rows), :] = both

    def gate_window(other):
        start = pl.multiple_of(other * piece // window * window, window)
        return gate_ref.at[:, pl.ds(start, window)]

    def send_gate(other):
        pltpu.make_async_remote_copy(
            src_ref=gate_window(other),
            dst_ref=gates_in.at[me],
            send_sem=gate_send_sem,
            recv_sem=gate_recv_sem,
            device_id=place(other),
            device_id_type=MESH,
        ).start()

    def send_rows(step, row0, rows):
        seq = sequence_at(step, seq_me, seqs)
        sub = min(piece, rows)
        for head in range(heads):
            for piece_row in range(0, rows, sub):
                row = pl.multiple_of(row0 + piece_row, sub)
                slot = row // piece
                to_sp = seq * classes + slot // halves
                to_tp = head * halves + slot % halves
                dest = to_sp * tp_count + to_tp
                landing = pl.multiple_of(me * piece + row % piece, sub)
                source = staging.at[seq * heads + head, pl.ds(row, sub), :]
                target = cache_ref.at[pl.ds(landing, sub), :]

                @pl.when(dest != me)
                def _():
                    pltpu.make_async_remote_copy(
                        src_ref=source,
                        dst_ref=target,
                        send_sem=send_sem,
                        recv_sem=recv_sem,
                        device_id={"sp": to_sp, "tp": to_tp},
                        device_id_type=MESH,
                    ).start()

                @pl.when(dest == me)
                def _():
                    pltpu.make_async_copy(source, target, own_sem).start()

    def send_tiles(first, last):
        def visit(index, carry):
            send_rows(index // tiles, index % tiles * tile, tile)
            return carry

        lax.fori_loop(first, last, visit, 0)

    def wait_bytes(ref, sem):
        pltpu.make_async_copy(ref, ref, sem).wait()

    gain_copy.wait()
    ramp_copy(0).wait()
    normalize(0, 0, ramp)
    k_copy.wait()
    v_copy.wait()
    for index in range(1, seqs * tiles):
        token_copy(index).start()
    multiply(0, 0, ramp)
    gate_copy.wait()
    pl.semaphore_wait(barrier, devices - 1)
    for_others(send_gate)
    send_rows(0, 0, ramp)
    ramp_copy(1).wait()
    normalize(0, ramp, ramp)
    multiply(0, ramp, ramp)
    send_rows(0, ramp, ramp)

    def project(index, carry):
        step, part = index // tiles, index % tiles
        row0 = pl.multiple_of(part * tile, tile)
        token_copy(index).wait()
        normalize(step, row0, tile)
        multiply(step, row0, tile)

        @pl.when((index < tiles) | (edge & (index < early)))
        def _():
            send_rows(step, row0, tile)

        return carry

    lax.fori_loop(1, seqs * tiles, project, 0)

    query_copy.wait()
    group = query_ref.shape[2]
    gates_in[me] = gate_ref[:, pl.ds(pl.multiple_of(me * piece // window * window, window), window)]
    other_gates = gates_in.at[pl.ds(0, devices - 1)]
    wait_bytes(other_gates, gate_recv_sem)
    lane = lax.broadcasted_iota(jnp.int32, (group, 2 * HD), 1)
    line = lax.broadcasted_iota(jnp.int32, (group, 2 * HD), 0)
    half = group // 2

    def pack(ref, top, total, out):
        folded = jnp.concatenate([out[:half], out[half:]], axis=1)
        stats = jnp.where(lane == line, top, 0.0) + jnp.where(lane == line + group, total, 0.0)
        for k in range(half):
            ref[:, k * 2 * HD : (k + 1) * 2 * HD] = folded[k : k + 1]
        ref[:, half * 2 * HD :] = jnp.sum(stats, axis=0, keepdims=True)

    def unpack(ref):
        rows = [ref[:, k * 2 * HD : (k + 1) * 2 * HD] for k in range(half + 1)]
        out = jnp.concatenate([r[:, :HD] for r in rows[:half]] + [r[:, HD:] for r in rows[:half]])
        top = jnp.sum(jnp.where(lane == line, rows[half], 0.0), axis=1, keepdims=True)
        total = jnp.sum(jnp.where(lane == line + group, rows[half], 0.0), axis=1, keepdims=True)
        return top, total, out

    def merge(left, right):
        best = jnp.maximum(left[0], right[0])
        scale_left, scale_right = jnp.exp(left[0] - best), jnp.exp(right[0] - best)
        total = left[1] * scale_left + right[1] * scale_right
        return best, total, left[2] * scale_left + right[2] * scale_right

    def attend(seq, carry):
        for head in range(heads):
            query = query_ref[seq, head]
            query = jnp.concatenate([query, jnp.zeros_like(query)], axis=1)
            for slot in range(classes * halves):
                to_sp = seq * classes + slot // halves
                to_tp = head * halves + slot % halves
                block = staging[seq * heads + head, slot * piece : (slot + 1) * piece, :]
                gates = gates_in[to_sp * tp_count + to_tp]
                choices = [gates[:, k * piece : (k + 1) * piece] for k in range(window // piece)]
                gate = choices[0]
                for k in range(1, len(choices)):
                    gate = jnp.where(me % (window // piece) == k, choices[k], gate)
                scores = lax.dot_general(
                    query, block, (((1,), (1,)), ((), ())), preferred_element_type=jnp.float32
                )
                scores = scores * HD ** (-0.5) - gate
                top = jnp.max(scores, axis=1, keepdims=True)
                weights = jnp.exp(scores - top)
                total = jnp.sum(weights, axis=1, keepdims=True)
                first = weights.astype(jnp.bfloat16).astype(jnp.float32)
                rest = weights - first
                second = rest.astype(jnp.bfloat16).astype(jnp.float32)
                stacked = jnp.concatenate([first, second, rest - second], axis=0)
                summed = jnp.dot(
                    stacked.astype(jnp.bfloat16), block, preferred_element_type=jnp.float32
                )
                summed = summed[:group] + summed[group : 2 * group] + summed[2 * group :]
                pack(own_parts.at[to_tp, to_sp], top, total, summed[:, HD:])
        return carry

    lax.fori_loop(0, seqs, attend, 0)

    def exchange(stage, source, target, device):
        pltpu.make_async_remote_copy(
            src_ref=source,
            dst_ref=target,
            send_sem=stage_send_sem.at[stage],
            recv_sem=stage_recv_sem.at[stage],
            device_id=device,
            device_id_type=MESH,
        ).start()

    plane = plane_parts.at[pl.ds(0, tp_count - 1)]
    along = line_parts.at[pl.ds(0, sp_count - 1)]

    for_plane(lambda t: exchange(0, own_parts.at[t], plane_parts.at[tp], {"tp": t}))
    plane_parts[tp] = own_parts[tp]
    wait_bytes(plane, stage_recv_sem.at[0])

    def merge_plane(s, carry):
        merged = functools.reduce(merge, [unpack(plane_parts.at[t, s]) for t in range(tp_count)])
        pack(merged_parts.at[s], *merged)
        return carry

    lax.fori_loop(0, sp_count, merge_plane, 0)
    for_line(lambda s: exchange(1, merged_parts.at[s], line_parts.at[sp], {"sp": s}))
    line_parts[sp] = merged_parts[sp]

    @pl.when(~edge)
    def _():
        send_tiles(tiles, early)

    wait_bytes(along, stage_recv_sem.at[1])
    merged = lax.fori_loop(
        1, sp_count, lambda s, kept: merge(kept, unpack(line_parts.at[s])), unpack(line_parts.at[0])
    )
    pack(finals.at[tp, sp], *merged)
    mine = finals.at[tp, sp]
    for_line(lambda s: exchange(2, mine, mine, {"sp": s}))

    @pl.when(~edge)
    def _():
        send_tiles(early, last)

    wait_bytes(along, stage_recv_sem.at[2])
    for_plane(lambda t: exchange(3, finals.at[tp], finals.at[tp], {"tp": t}))

    @pl.when(edge)
    def _():
        send_tiles(early, last)

    send_tiles(last, seqs * tiles)
    wait_bytes(plane, stage_recv_sem.at[3])
    for seq in range(seqs):
        for head in range(heads):
            slots = [
                unpack(finals.at[head * halves + b, seq * classes + c])
                for c in range(classes)
                for b in range(halves)
            ]
            _, total, out = functools.reduce(merge, slots)
            read_ref[seq, pl.ds(head * group, group), :] = out / total
    wait_bytes(other_gates, gate_send_sem)
    wait_bytes(plane, stage_send_sem.at[0])
    wait_bytes(along, stage_send_sem.at[1])
    wait_bytes(along, stage_send_sem.at[2])
    wait_bytes(plane, stage_send_sem.at[3])
    wait_bytes(cache_ref.at[pl.ds(0, piece), :], own_sem)
    sent = cache_ref.at[pl.ds(0, (devices - 1) * piece), :]
    wait_bytes(sent, send_sem)
    wait_bytes(sent, recv_sem)


def settle(cache_in, read_in, cache_out, read_out, sems):
    copies = [
        pltpu.make_async_copy(cache_in, cache_out, sems.at[0]),
        pltpu.make_async_copy(read_in, read_out, sems.at[1]),
    ]
    for copy in copies:
        copy.start()
    for copy in copies:
        copy.wait()


def solution(mesh):
    sp_count, tp_count = mesh.shape["sp"], mesh.shape["tp"]
    devices = sp_count * tp_count

    def shards(tokens, norm_gain, w_key, w_value, new_query, cum_gate):
        seqs, positions, width = tokens.shape
        heads = w_key.shape[1] // HD
        columns = w_key.shape[1]
        query_heads = new_query.shape[1]
        group = query_heads // heads
        length = cum_gate.shape[-1]
        tile = min(TILE, positions)
        part = (group // 2 + 1) * 2 * HD
        sizes = (sp_count, tp_count, seqs, heads, positions, width)
        vmem = pl.BlockSpec(memory_space=pltpu.VMEM)
        anywhere = pl.BlockSpec(memory_space=pltpu.HBM)
        cache, first_read = pl.pallas_call(
            functools.partial(kernel, sizes),
            out_shape=(
                pltpu.VMEM((length, 2 * HD), jnp.bfloat16),
                pltpu.VMEM((seqs, query_heads, HD), jnp.float32),
            ),
            in_specs=[anywhere] * 6,
            out_specs=(vmem, vmem),
            scratch_shapes=[
                pltpu.VMEM((seqs, positions, width), jnp.bfloat16),
                pltpu.VMEM((width, columns), jnp.bfloat16),
                pltpu.VMEM((width, columns), jnp.bfloat16),
                pltpu.VMEM((1, width), jnp.float32),
                pltpu.VMEM((seqs, heads, group, HD), jnp.bfloat16),
                pltpu.VMEM((1, length), jnp.float32),
                pltpu.VMEM((tile, width), jnp.bfloat16),
                pltpu.VMEM((seqs * heads, positions, 2 * HD), jnp.bfloat16),
                pltpu.VMEM((devices, 1, max(length // devices, 128)), jnp.float32),
                pltpu.VMEM((tp_count, sp_count, 1, part), jnp.float32),
                pltpu.VMEM((tp_count, sp_count, 1, part), jnp.float32),
                pltpu.VMEM((sp_count, 1, part), jnp.float32),
                pltpu.VMEM((sp_count, 1, part), jnp.float32),
                pltpu.VMEM((tp_count, sp_count, 1, part), jnp.float32),
                pltpu.SemaphoreType.DMA((seqs, positions // tile)),
                pltpu.SemaphoreType.DMA((2,)),
                pltpu.SemaphoreType.DMA((5,)),
                *[pltpu.SemaphoreType.DMA] * 4,
                pltpu.SemaphoreType.DMA((4,)),
                pltpu.SemaphoreType.DMA((4,)),
                pltpu.SemaphoreType.DMA,
            ],
            compiler_params=pltpu.CompilerParams(
                collective_id=0, has_side_effects=True, vmem_limit_bytes=VMEM_BYTES
            ),
        )(
            tokens,
            norm_gain.reshape(1, width),
            w_key,
            w_value,
            new_query.reshape(seqs, heads, group, HD),
            cum_gate.reshape(1, length),
        )
        cache, first_read = pl.pallas_call(
            settle,
            out_shape=(
                jax.ShapeDtypeStruct(cache.shape, cache.dtype),
                jax.ShapeDtypeStruct(first_read.shape, first_read.dtype),
            ),
            in_specs=[vmem] * 2,
            out_specs=(anywhere, anywhere),
            scratch_shapes=[pltpu.SemaphoreType.DMA((2,))],
            compiler_params=pltpu.CompilerParams(vmem_limit_bytes=VMEM_BYTES),
        )(
            pltpu.with_memory_space_constraint(cache, pltpu.VMEM),
            pltpu.with_memory_space_constraint(first_read, pltpu.VMEM),
        )
        return cache.reshape(1, 1, length, 2 * HD), first_read

    in_specs = (
        P("gr", ("sp", "tp"), None),
        P(),
        P(),
        P(),
        P("gr", None, None),
        P(("gr", "sp"), "tp", None),
    )
    out_specs = (P(("gr", "sp"), "tp", None, None), P("gr", None, None))
    return jax.shard_map(shards, mesh=mesh, in_specs=in_specs, out_specs=out_specs, check_vma=False)
```

```python
import functools

import jax
import jax.numpy as jnp
from jax import lax
from jax.experimental import pallas as pl
from jax.experimental.pallas import tpu as pltpu
from jax.sharding import PartitionSpec as P

HD = 64
NORM_FLOOR = 0.05
SCORE_FLOOR = -1e30
MESH = pl.DeviceIdType.MESH
TILE = 256
NORM_ROWS = 16
VMEM_BYTES = 60_000_000


def is_edge(own, count):
    return (own == 0) | (own == count - 1) | (count < 4)


def sequence_at(step, own, count):
    low = own < count // 2
    moved = jnp.where(step == 0, count - 2, jnp.where(step <= count - 2, step - 1, step))
    turn = jnp.where(is_edge(own, count), moved, step)
    first = jnp.where(low, count - 1 - turn, turn)
    following = jnp.where(low, count - 2 - turn, turn + 1)
    own_step = jnp.where(low, count - 1 - own, own)
    shifted = jnp.where(turn >= own_step, following, first)
    return jnp.where(step == count - 1, own, shifted)


def kernel(
    sizes,
    tokens_hbm,
    gain_hbm,
    wk_hbm,
    wv_hbm,
    query_hbm,
    gate_hbm,
    cache_ref,
    read_ref,
    tok_buf,
    wk_buf,
    wv_buf,
    gain_ref,
    query_ref,
    gate_ref,
    norm_buf,
    staging,
    gates_in,
    own_parts,
    plane_parts,
    merged_parts,
    line_parts,
    finals,
    tok_sem,
    ramp_sem,
    w_sem,
    send_sem,
    recv_sem,
    gate_send_sem,
    gate_recv_sem,
    stage_send_sem,
    stage_recv_sem,
    own_sem,
    ready,
):
    sp_count, tp_count, seqs, heads, positions, width = sizes
    devices = sp_count * tp_count
    classes, halves = sp_count // seqs, tp_count // heads
    piece = positions // (classes * halves)
    sp, tp = lax.axis_index("sp"), lax.axis_index("tp")
    me = sp * tp_count + tp
    seq_me, head_me = sp // classes, tp // halves
    tile = min(TILE, positions)
    tiles = positions // tile
    half_tile = tile // 2
    ramp = tile // 4
    window = max(piece, 128)
    edge = is_edge(seq_me, seqs)
    edge_devices = devices if seqs < 4 else 2 * classes * tp_count
    lead = max(tiles // 2, 1)
    last = (seqs - 1) * tiles
    units = seqs * tiles

    def place(other):
        return {"sp": other // tp_count, "tp": other % tp_count}

    def for_others(body):
        def visit(other, carry):
            @pl.when(other != me)
            def _():
                body(other)

            return carry

        lax.fori_loop(0, devices, visit, 0)

    def for_line(body):
        def visit(other, carry):
            @pl.when(other != sp)
            def _():
                body(other)

            return carry

        lax.fori_loop(0, sp_count, visit, 0)

    def for_plane(body):
        def visit(other, carry):
            @pl.when(other != tp)
            def _():
                body(other)

            return carry

        lax.fori_loop(0, tp_count, visit, 0)

    def unit_at(unit):
        ahead = unit == 0
        step = jnp.where(ahead, 1, jnp.where(unit <= tiles, 0, unit // tiles))
        part = jnp.where(ahead, 0, jnp.where(unit <= tiles, unit - 1, unit % tiles))
        step = jnp.where(edge, unit // tiles, step)
        part = jnp.where(edge, unit % tiles, part)
        return sequence_at(step, seq_me, seqs), pl.multiple_of(part * tile, tile)

    def rows_copy(unit, row, rows, sem):
        seq, row0 = unit_at(unit)
        source = tokens_hbm.at[seq, pl.ds(row0 + row, rows), :]
        return pltpu.make_async_copy(source, tok_buf.at[unit, pl.ds(row, rows), :], sem)

    def ramp_copy(part):
        if part:
            return rows_copy(0, ramp, tile - ramp, ramp_sem.at[1])
        return rows_copy(0, 0, ramp, ramp_sem.at[0])

    def token_copy(unit):
        return rows_copy(unit, 0, tile, tok_sem.at[unit])

    k_copy = pltpu.make_async_copy(wk_hbm, wk_buf, w_sem.at[0])
    v_copy = pltpu.make_async_copy(wv_hbm, wv_buf, w_sem.at[1])
    gain_copy = pltpu.make_async_copy(gain_hbm, gain_ref, w_sem.at[2])
    query_copy = pltpu.make_async_copy(query_hbm, query_ref, w_sem.at[3])
    gate_copy = pltpu.make_async_copy(gate_hbm, gate_ref, w_sem.at[4])
    ramp_copy(0).start()
    gain_copy.start()
    gate_copy.start()
    k_copy.start()
    v_copy.start()
    ramp_copy(1).start()

    barrier = pltpu.get_barrier_semaphore()

    def on_edge(other):
        return is_edge(other // tp_count // classes, seqs)

    def greet(other):
        pl.semaphore_signal(barrier, inc=1, device_id=place(other), device_id_type=MESH)

    def greet_edge(other):
        @pl.when(on_edge(other))
        def _():
            greet(other)

    def answer(other):
        @pl.when(~on_edge(other))
        def _():
            pl.semaphore_signal(ready, inc=1, device_id=place(other), device_id_type=MESH)

    @pl.when(edge)
    def _():
        for_others(greet_edge)

    @pl.when(~edge)
    def _():
        for_others(greet)

    query_copy.start()

    def normalize(unit, row, rows):
        gain = gain_ref[...]
        for piece_row in range(0, rows, NORM_ROWS):
            block = tok_buf[unit, row + piece_row : row + piece_row + NORM_ROWS, :]
            block = block.astype(jnp.float32)
            mean = jnp.mean(block * block, axis=-1, keepdims=True)
            normed = block * lax.rsqrt(mean + NORM_FLOOR) * gain
            norm_buf[pl.ds(piece_row, NORM_ROWS), :] = normed.astype(jnp.bfloat16)

    def multiply(unit, row, rows):
        seq, row0 = unit_at(unit)
        normed_tile = norm_buf[:rows, :]
        keys = jnp.dot(normed_tile, wk_buf[...], preferred_element_type=jnp.float32)
        values = jnp.dot(normed_tile, wv_buf[...], preferred_element_type=jnp.float32)
        keys = keys.astype(jnp.bfloat16)
        values = values.astype(jnp.bfloat16)
        for head in range(heads):
            cols = slice(head * HD, (head + 1) * HD)
            both = jnp.concatenate([keys[:, cols], values[:, cols]], axis=1)
            staging[seq * heads + head, pl.ds(pl.multiple_of(row0 + row, ramp), rows), :] = both

    def gate_window(other):
        start = pl.multiple_of(other * piece // window * window, window)
        return gate_ref.at[:, pl.ds(start, window)]

    def send_gate(other):
        pltpu.make_async_remote_copy(
            src_ref=gate_window(other),
            dst_ref=gates_in.at[me],
            send_sem=gate_send_sem,
            recv_sem=gate_recv_sem,
            device_id=place(other),
            device_id_type=MESH,
        ).start()

    def send_gate_if(chosen):
        def visit(other):
            @pl.when(chosen(other))
            def _():
                send_gate(other)

        for_others(visit)

    def send_rows(unit, start, rows):
        seq, row0 = unit_at(unit)
        row0 = row0 + start
        sub = min(piece, rows)
        for head in range(heads):
            for piece_row in range(0, rows, sub):
                row = pl.multiple_of(row0 + piece_row, sub)
                slot = row // piece
                to_sp = seq * classes + slot // halves
                to_tp = head * halves + slot % halves
                dest = to_sp * tp_count + to_tp
                landing = pl.multiple_of(me * piece + row % piece, sub)
                source = staging.at[seq * heads + head, pl.ds(row, sub), :]
                target = cache_ref.at[pl.ds(landing, sub), :]

                @pl.when(dest != me)
                def _():
                    pltpu.make_async_remote_copy(
                        src_ref=source,
                        dst_ref=target,
                        send_sem=send_sem,
                        recv_sem=recv_sem,
                        device_id={"sp": to_sp, "tp": to_tp},
                        device_id_type=MESH,
                    ).start()

                @pl.when(dest == me)
                def _():
                    pltpu.make_async_copy(source, target, own_sem).start()

    def send_units(first, last, start=0, rows=tile):
        def visit(unit, carry):
            send_rows(unit, start, rows)
            return carry

        lax.fori_loop(first, last, visit, 0)

    def wait_bytes(ref, sem):
        pltpu.make_async_copy(ref, ref, sem).wait()

    gain_copy.wait()
    ramp_copy(0).wait()
    normalize(0, 0, ramp)
    gate_copy.wait()

    @pl.when(edge)
    def _():
        pl.semaphore_wait(barrier, devices - 1)
        for_others(answer)
        for_others(send_gate)

    @pl.when(~edge)
    def _():
        pl.semaphore_wait(barrier, devices - edge_devices - 1)
        send_gate_if(lambda other: ~on_edge(other))

    k_copy.wait()
    v_copy.wait()
    for unit in range(1, units):
        token_copy(unit).start()
    multiply(0, 0, ramp)
    send_rows(0, 0, ramp)
    ramp_copy(1).wait()
    normalize(0, ramp, tile - ramp)
    multiply(0, ramp, tile - ramp)
    send_rows(0, ramp, ramp)
    send_rows(0, half_tile, half_tile)

    def project(unit, carry):
        token_copy(unit).wait()
        normalize(unit, 0, tile)
        multiply(unit, 0, tile)

        @pl.when((unit == 1) & ~edge)
        def _():
            pl.semaphore_wait(ready, edge_devices)
            send_gate_if(on_edge)

        @pl.when((unit < jnp.where(edge, lead, tiles)) | (edge & (unit // lead * lead == tiles)))
        def _():
            send_rows(unit, 0, tile)

        @pl.when(edge & (unit == tiles + lead))
        def _():
            send_units(lead, tiles)

        @pl.when(~edge & (unit == tiles + 1))
        def _():
            send_units(tiles, 2 * tiles - 1, 0, half_tile)

        return carry

    lax.fori_loop(1, units, project, 0)

    query_copy.wait()
    group = query_ref.shape[2]
    gates_in[me] = gate_ref[:, pl.ds(pl.multiple_of(me * piece // window * window, window), window)]
    other_gates = gates_in.at[pl.ds(0, devices - 1)]
    wait_bytes(other_gates, gate_recv_sem)
    lane = lax.broadcasted_iota(jnp.int32, (group, 2 * HD), 1)
    line = lax.broadcasted_iota(jnp.int32, (group, 2 * HD), 0)
    half = group // 2

    def pack(ref, top, total, out):
        folded = jnp.concatenate([out[:half], out[half:]], axis=1)
        stats = jnp.where(lane == line, top, 0.0) + jnp.where(lane == line + group, total, 0.0)
        for k in range(half):
            ref[:, k * 2 * HD : (k + 1) * 2 * HD] = folded[k : k + 1]
        ref[:, half * 2 * HD :] = jnp.sum(stats, axis=0, keepdims=True)

    def unpack(ref):
        rows = [ref[:, k * 2 * HD : (k + 1) * 2 * HD] for k in range(half + 1)]
        out = jnp.concatenate([r[:, :HD] for r in rows[:half]] + [r[:, HD:] for r in rows[:half]])
        top = jnp.sum(jnp.where(lane == line, rows[half], 0.0), axis=1, keepdims=True)
        total = jnp.sum(jnp.where(lane == line + group, rows[half], 0.0), axis=1, keepdims=True)
        return top, total, out

    def merge(left, right):
        best = jnp.maximum(left[0], right[0])
        scale_left, scale_right = jnp.exp(left[0] - best), jnp.exp(right[0] - best)
        total = left[1] * scale_left + right[1] * scale_right
        return best, total, left[2] * scale_left + right[2] * scale_right

    def attend(seq, carry):
        for head in range(heads):
            query = query_ref[seq, head]
            query = jnp.concatenate([query, jnp.zeros_like(query)], axis=1)
            for slot in range(classes * halves):
                to_sp = seq * classes + slot // halves
                to_tp = head * halves + slot % halves
                block = staging[seq * heads + head, slot * piece : (slot + 1) * piece, :]
                gates = gates_in[to_sp * tp_count + to_tp]
                choices = [gates[:, k * piece : (k + 1) * piece] for k in range(window // piece)]
                gate = choices[0]
                for k in range(1, len(choices)):
                    gate = jnp.where(me % (window // piece) == k, choices[k], gate)
                scores = lax.dot_general(
                    query, block, (((1,), (1,)), ((), ())), preferred_element_type=jnp.float32
                )
                scores = scores * HD ** (-0.5) - gate
                top = jnp.max(scores, axis=1, keepdims=True)
                weights = jnp.exp(scores - top)
                total = jnp.sum(weights, axis=1, keepdims=True)
                first = weights.astype(jnp.bfloat16).astype(jnp.float32)
                rest = weights - first
                second = rest.astype(jnp.bfloat16).astype(jnp.float32)
                stacked = jnp.concatenate([first, second, rest - second], axis=0)
                summed = jnp.dot(
                    stacked.astype(jnp.bfloat16), block, preferred_element_type=jnp.float32
                )
                summed = summed[:group] + summed[group : 2 * group] + summed[2 * group :]
                pack(own_parts.at[to_tp, to_sp], top, total, summed[:, HD:])
        return carry

    lax.fori_loop(0, seqs, attend, 0)

    def exchange(stage, source, target, device):
        pltpu.make_async_remote_copy(
            src_ref=source,
            dst_ref=target,
            send_sem=stage_send_sem.at[stage],
            recv_sem=stage_recv_sem.at[stage],
            device_id=device,
            device_id_type=MESH,
        ).start()

    plane = plane_parts.at[pl.ds(0, tp_count - 1)]
    along = line_parts.at[pl.ds(0, sp_count - 1)]

    for_plane(lambda t: exchange(0, own_parts.at[t], plane_parts.at[tp], {"tp": t}))
    plane_parts[tp] = own_parts[tp]
    wait_bytes(plane, stage_recv_sem.at[0])

    def merge_plane(s, carry):
        merged = functools.reduce(merge, [unpack(plane_parts.at[t, s]) for t in range(tp_count)])
        pack(merged_parts.at[s], *merged)
        return carry

    lax.fori_loop(0, sp_count, merge_plane, 0)
    for_line(lambda s: exchange(1, merged_parts.at[s], line_parts.at[sp], {"sp": s}))
    line_parts[sp] = merged_parts[sp]

    @pl.when(~edge)
    def _():
        send_units(tiles, 2 * tiles - 1, half_tile, half_tile)

    send_units(last, units)
    wait_bytes(along, stage_recv_sem.at[1])
    merged = lax.fori_loop(
        1, sp_count, lambda s, kept: merge(kept, unpack(line_parts.at[s])), unpack(line_parts.at[0])
    )
    pack(finals.at[tp, sp], *merged)
    mine = finals.at[tp, sp]
    for_line(lambda s: exchange(2, mine, mine, {"sp": s}))

    @pl.when(~edge)
    def _():
        send_units(2 * tiles - 1, last)

    wait_bytes(along, stage_recv_sem.at[2])
    for_plane(lambda t: exchange(3, finals.at[tp], finals.at[tp], {"tp": t}))

    @pl.when(edge)
    def _():
        send_units(tiles + lead, last)

    wait_bytes(plane, stage_recv_sem.at[3])
    for seq in range(seqs):
        for head in range(heads):
            slots = [
                unpack(finals.at[head * halves + b, seq * classes + c])
                for c in range(classes)
                for b in range(halves)
            ]
            _, total, out = functools.reduce(merge, slots)
            read_ref[seq, pl.ds(head * group, group), :] = out / total
    wait_bytes(other_gates, gate_send_sem)
    wait_bytes(plane, stage_send_sem.at[0])
    wait_bytes(along, stage_send_sem.at[1])
    wait_bytes(along, stage_send_sem.at[2])
    wait_bytes(plane, stage_send_sem.at[3])
    wait_bytes(cache_ref.at[pl.ds(0, piece), :], own_sem)
    sent = cache_ref.at[pl.ds(0, (devices - 1) * piece), :]
    wait_bytes(sent, send_sem)
    wait_bytes(sent, recv_sem)


def settle(cache_in, read_in, cache_out, read_out, sems):
    copies = [
        pltpu.make_async_copy(cache_in, cache_out, sems.at[0]),
        pltpu.make_async_copy(read_in, read_out, sems.at[1]),
    ]
    for copy in copies:
        copy.start()
    for copy in copies:
        copy.wait()


def solution(mesh):
    sp_count, tp_count = mesh.shape["sp"], mesh.shape["tp"]
    devices = sp_count * tp_count

    def shards(tokens, norm_gain, w_key, w_value, new_query, cum_gate):
        seqs, positions, width = tokens.shape
        heads = w_key.shape[1] // HD
        columns = w_key.shape[1]
        query_heads = new_query.shape[1]
        group = query_heads // heads
        length = cum_gate.shape[-1]
        tile = min(TILE, positions)
        part = (group // 2 + 1) * 2 * HD
        sizes = (sp_count, tp_count, seqs, heads, positions, width)
        vmem = pl.BlockSpec(memory_space=pltpu.VMEM)
        anywhere = pl.BlockSpec(memory_space=pltpu.HBM)
        cache, first_read = pl.pallas_call(
            functools.partial(kernel, sizes),
            out_shape=(
                pltpu.VMEM((length, 2 * HD), jnp.bfloat16),
                pltpu.VMEM((seqs, query_heads, HD), jnp.float32),
            ),
            in_specs=[anywhere] * 6,
            out_specs=(vmem, vmem),
            scratch_shapes=[
                pltpu.VMEM((seqs * positions // tile, tile, width), jnp.bfloat16),
                pltpu.VMEM((width, columns), jnp.bfloat16),
                pltpu.VMEM((width, columns), jnp.bfloat16),
                pltpu.VMEM((1, width), jnp.float32),
                pltpu.VMEM((seqs, heads, group, HD), jnp.bfloat16),
                pltpu.VMEM((1, length), jnp.float32),
                pltpu.VMEM((tile, width), jnp.bfloat16),
                pltpu.VMEM((seqs * heads, positions, 2 * HD), jnp.bfloat16),
                pltpu.VMEM((devices, 1, max(length // devices, 128)), jnp.float32),
                pltpu.VMEM((tp_count, sp_count, 1, part), jnp.float32),
                pltpu.VMEM((tp_count, sp_count, 1, part), jnp.float32),
                pltpu.VMEM((sp_count, 1, part), jnp.float32),
                pltpu.VMEM((sp_count, 1, part), jnp.float32),
                pltpu.VMEM((tp_count, sp_count, 1, part), jnp.float32),
                pltpu.SemaphoreType.DMA((seqs * positions // tile,)),
                pltpu.SemaphoreType.DMA((2,)),
                pltpu.SemaphoreType.DMA((5,)),
                *[pltpu.SemaphoreType.DMA] * 4,
                pltpu.SemaphoreType.DMA((4,)),
                pltpu.SemaphoreType.DMA((4,)),
                pltpu.SemaphoreType.DMA,
                pltpu.SemaphoreType.REGULAR,
            ],
            compiler_params=pltpu.CompilerParams(
                collective_id=0, has_side_effects=True, vmem_limit_bytes=VMEM_BYTES
            ),
        )(
            tokens,
            norm_gain.reshape(1, width),
            w_key,
            w_value,
            new_query.reshape(seqs, heads, group, HD),
            cum_gate.reshape(1, length),
        )
        cache, first_read = pl.pallas_call(
            settle,
            out_shape=(
                jax.ShapeDtypeStruct(cache.shape, cache.dtype),
                jax.ShapeDtypeStruct(first_read.shape, first_read.dtype),
            ),
            in_specs=[vmem] * 2,
            out_specs=(anywhere, anywhere),
            scratch_shapes=[pltpu.SemaphoreType.DMA((2,))],
            compiler_params=pltpu.CompilerParams(vmem_limit_bytes=VMEM_BYTES),
        )(
            pltpu.with_memory_space_constraint(cache, pltpu.VMEM),
            pltpu.with_memory_space_constraint(first_read, pltpu.VMEM),
        )
        return cache.reshape(1, 1, length, 2 * HD), first_read

    in_specs = (
        P("gr", ("sp", "tp"), None),
        P(),
        P(),
        P(),
        P("gr", None, None),
        P(("gr", "sp"), "tp", None),
    )
    out_specs = (P(("gr", "sp"), "tp", None, None), P("gr", None, None))
    return jax.shard_map(shards, mesh=mesh, in_specs=in_specs, out_specs=out_specs, check_vma=False)
```

```python
import functools

import jax
import jax.numpy as jnp
from jax import lax
from jax.experimental import pallas as pl
from jax.experimental.pallas import tpu as pltpu
from jax.sharding import PartitionSpec as P

HD = 64
NORM_FLOOR = 0.05
SCORE_FLOOR = -1e30
MESH = pl.DeviceIdType.MESH
TILE = 256
NORM_ROWS = 16
VMEM_BYTES = 60_000_000


def has_middle(count):
    return count >= 4 and count % 2 == 0


def is_edge(own, count):
    return (own == 0) | (own == count - 1) | (not has_middle(count))


def sequence_at(step, own, count):
    low = own < count // 2
    moved = jnp.where(step == 0, count - 2, jnp.where(step <= count - 2, step - 1, step))
    turn = jnp.where(is_edge(own, count), moved, step)
    first = jnp.where(low, count - 1 - turn, turn)
    following = jnp.where(low, count - 2 - turn, turn + 1)
    own_step = jnp.where(low, count - 1 - own, own)
    shifted = jnp.where(turn >= own_step, following, first)
    return jnp.where(step == count - 1, own, shifted)


def kernel(
    sizes,
    tokens_hbm,
    gain_hbm,
    wk_hbm,
    wv_hbm,
    query_hbm,
    gate_hbm,
    cache_ref,
    read_ref,
    tok_buf,
    wk_buf,
    wv_buf,
    gain_ref,
    query_ref,
    gate_ref,
    norm_buf,
    staging,
    gates_in,
    own_parts,
    plane_parts,
    merged_parts,
    line_parts,
    finals,
    tok_sem,
    ramp_sem,
    w_sem,
    send_sem,
    recv_sem,
    gate_send_sem,
    gate_recv_sem,
    stage_send_sem,
    stage_recv_sem,
    own_sem,
    ready,
):
    sp_count, tp_count, seqs, heads, positions, width = sizes
    devices = sp_count * tp_count
    classes, halves = sp_count // seqs, tp_count // heads
    piece = positions // (classes * halves)
    sp, tp = lax.axis_index("sp"), lax.axis_index("tp")
    me = sp * tp_count + tp
    seq_me, head_me = sp // classes, tp // halves
    tile = min(TILE, positions)
    tiles = positions // tile
    half_tile = tile // 2
    ramp = tile // 4
    window = max(piece, 128)
    edge = is_edge(seq_me, seqs)
    edge_devices = 2 * classes * tp_count if has_middle(seqs) else devices
    lead = max(tiles // 2, 1)
    last = (seqs - 1) * tiles
    units = seqs * tiles

    def place(other):
        return {"sp": other // tp_count, "tp": other % tp_count}

    def for_others(body):
        def visit(other, carry):
            @pl.when(other != me)
            def _():
                body(other)

            return carry

        lax.fori_loop(0, devices, visit, 0)

    def for_line(body):
        def visit(other, carry):
            @pl.when(other != sp)
            def _():
                body(other)

            return carry

        lax.fori_loop(0, sp_count, visit, 0)

    def for_plane(body):
        def visit(other, carry):
            @pl.when(other != tp)
            def _():
                body(other)

            return carry

        lax.fori_loop(0, tp_count, visit, 0)

    def unit_at(unit):
        ahead = unit == 0
        step = jnp.where(ahead, 1, jnp.where(unit <= tiles, 0, unit // tiles))
        part = jnp.where(ahead, 0, jnp.where(unit <= tiles, unit - 1, unit % tiles))
        step = jnp.where(edge, unit // tiles, step)
        part = jnp.where(edge, unit % tiles, part)
        return sequence_at(step, seq_me, seqs), pl.multiple_of(part * tile, tile)

    def rows_copy(unit, row, rows, sem):
        seq, row0 = unit_at(unit)
        source = tokens_hbm.at[seq, pl.ds(row0 + row, rows), :]
        return pltpu.make_async_copy(source, tok_buf.at[unit, pl.ds(row, rows), :], sem)

    def ramp_copy(part):
        if part:
            return rows_copy(0, ramp, tile - ramp, ramp_sem.at[1])
        return rows_copy(0, 0, ramp, ramp_sem.at[0])

    def token_copy(unit):
        return rows_copy(unit, 0, tile, tok_sem.at[unit])

    k_copy = pltpu.make_async_copy(wk_hbm, wk_buf, w_sem.at[0])
    v_copy = pltpu.make_async_copy(wv_hbm, wv_buf, w_sem.at[1])
    gain_copy = pltpu.make_async_copy(gain_hbm, gain_ref, w_sem.at[2])
    query_copy = pltpu.make_async_copy(query_hbm, query_ref, w_sem.at[3])
    gate_copy = pltpu.make_async_copy(gate_hbm, gate_ref, w_sem.at[4])
    def on_edge(other):
        return is_edge(other // tp_count // classes, seqs)

    def greet(other):
        pl.semaphore_signal(barrier, inc=1, device_id=place(other), device_id_type=MESH)

    def answer(other):
        @pl.when(~on_edge(other))
        def _():
            pl.semaphore_signal(ready, inc=1, device_id=place(other), device_id_type=MESH)

    upper = seq_me >= seqs // 2
    plane_size = classes * tp_count
    across_first = jnp.where(upper, 1, seqs // 2) * plane_size
    across_count = (seqs // 2 - 1) * plane_size
    barrier = pltpu.get_barrier_semaphore()

    def is_across(other):
        return (other >= across_first) & (other < across_first + across_count)

    def greet_across(index, carry):
        greet(across_first + index)
        return carry

    @pl.when(~edge)
    def _():
        lax.fori_loop(0, across_count, greet_across, 0)

    ramp_copy(0).start()
    gain_copy.start()
    gate_copy.start()
    k_copy.start()
    v_copy.start()

    for_others(lambda other: pl.when(on_edge(other))(lambda: greet(other)))
    query_copy.start()

    def normalize(unit, row, rows):
        gain = gain_ref[...]
        for piece_row in range(0, rows, NORM_ROWS):
            block = tok_buf[unit, row + piece_row : row + piece_row + NORM_ROWS, :]
            block = block.astype(jnp.float32)
            mean = jnp.mean(block * block, axis=-1, keepdims=True)
            normed = block * lax.rsqrt(mean + NORM_FLOOR) * gain
            norm_buf[pl.ds(piece_row, NORM_ROWS), :] = normed.astype(jnp.bfloat16)

    def multiply(unit, row, rows):
        seq, row0 = unit_at(unit)
        normed_tile = norm_buf[:rows, :]
        keys = jnp.dot(normed_tile, wk_buf[...], preferred_element_type=jnp.float32)
        values = jnp.dot(normed_tile, wv_buf[...], preferred_element_type=jnp.float32)
        keys = keys.astype(jnp.bfloat16)
        values = values.astype(jnp.bfloat16)
        for head in range(heads):
            cols = slice(head * HD, (head + 1) * HD)
            both = jnp.concatenate([keys[:, cols], values[:, cols]], axis=1)
            staging[seq * heads + head, pl.ds(pl.multiple_of(row0 + row, ramp), rows), :] = both

    def gate_window(other):
        start = pl.multiple_of(other * piece // window * window, window)
        return gate_ref.at[:, pl.ds(start, window)]

    def send_gate(other):
        pltpu.make_async_remote_copy(
            src_ref=gate_window(other),
            dst_ref=gates_in.at[me],
            send_sem=gate_send_sem,
            recv_sem=gate_recv_sem,
            device_id=place(other),
            device_id_type=MESH,
        ).start()

    def send_gate_if(chosen):
        def visit(other):
            @pl.when(chosen(other))
            def _():
                send_gate(other)

        for_others(visit)

    def send_rows(unit, start, rows):
        seq, row0 = unit_at(unit)
        row0 = row0 + start
        sub = min(piece, rows)
        for head in range(heads):
            for piece_row in range(0, rows, sub):
                row = pl.multiple_of(row0 + piece_row, sub)
                slot = row // piece
                to_sp = seq * classes + slot // halves
                to_tp = head * halves + slot % halves
                dest = to_sp * tp_count + to_tp
                landing = pl.multiple_of(me * piece + row % piece, sub)
                source = staging.at[seq * heads + head, pl.ds(row, sub), :]
                target = cache_ref.at[pl.ds(landing, sub), :]

                @pl.when(dest != me)
                def _():
                    pltpu.make_async_remote_copy(
                        src_ref=source,
                        dst_ref=target,
                        send_sem=send_sem,
                        recv_sem=recv_sem,
                        device_id={"sp": to_sp, "tp": to_tp},
                        device_id_type=MESH,
                    ).start()

                @pl.when(dest == me)
                def _():
                    pltpu.make_async_copy(source, target, own_sem).start()

    def send_units(first, last, start=0, rows=tile):
        def visit(unit, carry):
            send_rows(unit, start, rows)
            return carry

        lax.fori_loop(first, last, visit, 0)

    def wait_bytes(ref, sem):
        pltpu.make_async_copy(ref, ref, sem).wait()

    def open_links(chosen):
        @pl.when(chosen & edge)
        def _():
            pl.semaphore_wait(barrier, devices - 1)
            for_others(answer)
            for_others(send_gate)

        @pl.when(chosen & ~edge)
        def _():
            pl.semaphore_wait(barrier, across_count)
            send_gate_if(is_across)

    gate_copy.wait()
    open_links(upper)
    gain_copy.wait()
    ramp_copy(0).wait()
    normalize(0, 0, ramp)
    ramp_copy(1).start()
    k_copy.wait()
    v_copy.wait()
    for unit in range(1, units):
        token_copy(unit).start()
    multiply(0, 0, ramp)
    open_links(~upper)
    send_rows(0, 0, ramp)
    ramp_copy(1).wait()
    normalize(0, ramp, tile - ramp)
    multiply(0, ramp, tile - ramp)
    send_rows(0, ramp, ramp)
    send_rows(0, half_tile, half_tile)

    def project(unit, carry):
        token_copy(unit).wait()
        normalize(unit, 0, tile)
        multiply(unit, 0, tile)

        @pl.when((unit == 1) & ~edge)
        def _():
            pl.semaphore_wait(ready, edge_devices)
            send_gate_if(lambda other: ~is_across(other))

        @pl.when((unit < jnp.where(edge, lead, tiles)) | (edge & (unit // lead * lead == tiles)))
        def _():
            send_rows(unit, 0, tile)

        @pl.when(edge & (unit == tiles + lead))
        def _():
            send_units(lead, tiles)

        @pl.when(~edge & (unit == tiles + 1))
        def _():
            send_units(tiles, 2 * tiles - 1, 0, half_tile)

        return carry

    lax.fori_loop(1, units, project, 0)

    query_copy.wait()
    group = query_ref.shape[2]
    gates_in[me] = gate_ref[:, pl.ds(pl.multiple_of(me * piece // window * window, window), window)]
    other_gates = gates_in.at[pl.ds(0, devices - 1)]
    wait_bytes(other_gates, gate_recv_sem)
    lane = lax.broadcasted_iota(jnp.int32, (group, 2 * HD), 1)
    line = lax.broadcasted_iota(jnp.int32, (group, 2 * HD), 0)
    half = group // 2

    def pack(ref, top, total, out):
        folded = jnp.concatenate([out[:half], out[half:]], axis=1)
        stats = jnp.where(lane == line, top, 0.0) + jnp.where(lane == line + group, total, 0.0)
        for k in range(half):
            ref[:, k * 2 * HD : (k + 1) * 2 * HD] = folded[k : k + 1]
        ref[:, half * 2 * HD :] = jnp.sum(stats, axis=0, keepdims=True)

    def unpack(ref):
        rows = [ref[:, k * 2 * HD : (k + 1) * 2 * HD] for k in range(half + 1)]
        out = jnp.concatenate([r[:, :HD] for r in rows[:half]] + [r[:, HD:] for r in rows[:half]])
        top = jnp.sum(jnp.where(lane == line, rows[half], 0.0), axis=1, keepdims=True)
        total = jnp.sum(jnp.where(lane == line + group, rows[half], 0.0), axis=1, keepdims=True)
        return top, total, out

    def merge(left, right):
        best = jnp.maximum(left[0], right[0])
        scale_left, scale_right = jnp.exp(left[0] - best), jnp.exp(right[0] - best)
        total = left[1] * scale_left + right[1] * scale_right
        return best, total, left[2] * scale_left + right[2] * scale_right

    def attend(seq, carry):
        for head in range(heads):
            query = query_ref[seq, head]
            query = jnp.concatenate([query, jnp.zeros_like(query)], axis=1)
            for slot in range(classes * halves):
                to_sp = seq * classes + slot // halves
                to_tp = head * halves + slot % halves
                block = staging[seq * heads + head, slot * piece : (slot + 1) * piece, :]
                gates = gates_in[to_sp * tp_count + to_tp]
                choices = [gates[:, k * piece : (k + 1) * piece] for k in range(window // piece)]
                gate = choices[0]
                for k in range(1, len(choices)):
                    gate = jnp.where(me % (window // piece) == k, choices[k], gate)
                scores = lax.dot_general(
                    query, block, (((1,), (1,)), ((), ())), preferred_element_type=jnp.float32
                )
                scores = scores * HD ** (-0.5) - gate
                top = jnp.max(scores, axis=1, keepdims=True)
                weights = jnp.exp(scores - top)
                total = jnp.sum(weights, axis=1, keepdims=True)
                first = weights.astype(jnp.bfloat16).astype(jnp.float32)
                rest = weights - first
                second = rest.astype(jnp.bfloat16).astype(jnp.float32)
                stacked = jnp.concatenate([first, second, rest - second], axis=0)
                summed = jnp.dot(
                    stacked.astype(jnp.bfloat16), block, preferred_element_type=jnp.float32
                )
                summed = summed[:group] + summed[group : 2 * group] + summed[2 * group :]
                pack(own_parts.at[to_tp, to_sp], top, total, summed[:, HD:])
        return carry

    lax.fori_loop(0, seqs, attend, 0)

    def exchange(stage, source, target, device):
        pltpu.make_async_remote_copy(
            src_ref=source,
            dst_ref=target,
            send_sem=stage_send_sem.at[stage],
            recv_sem=stage_recv_sem.at[stage],
            device_id=device,
            device_id_type=MESH,
        ).start()

    plane = plane_parts.at[pl.ds(0, tp_count - 1)]
    along = line_parts.at[pl.ds(0, sp_count - 1)]

    for_plane(lambda t: exchange(0, own_parts.at[t], plane_parts.at[tp], {"tp": t}))
    plane_parts[tp] = own_parts[tp]
    wait_bytes(plane, stage_recv_sem.at[0])

    def merge_plane(s, carry):
        merged = functools.reduce(merge, [unpack(plane_parts.at[t, s]) for t in range(tp_count)])
        pack(merged_parts.at[s], *merged)
        return carry

    lax.fori_loop(0, sp_count, merge_plane, 0)
    for_line(lambda s: exchange(1, merged_parts.at[s], line_parts.at[sp], {"sp": s}))
    line_parts[sp] = merged_parts[sp]

    @pl.when(~edge)
    def _():
        send_units(tiles, 2 * tiles - 1, half_tile, half_tile)

    send_units(last, units)
    wait_bytes(along, stage_recv_sem.at[1])
    merged = lax.fori_loop(
        1, sp_count, lambda s, kept: merge(kept, unpack(line_parts.at[s])), unpack(line_parts.at[0])
    )
    pack(finals.at[tp, sp], *merged)
    mine = finals.at[tp, sp]
    for_line(lambda s: exchange(2, mine, mine, {"sp": s}))

    @pl.when(~edge)
    def _():
        send_units(2 * tiles - 1, last)

    wait_bytes(along, stage_recv_sem.at[2])
    for_plane(lambda t: exchange(3, finals.at[tp], finals.at[tp], {"tp": t}))

    @pl.when(edge)
    def _():
        send_units(tiles + lead, last)

    wait_bytes(plane, stage_recv_sem.at[3])
    for seq in range(seqs):
        for head in range(heads):
            slots = [
                unpack(finals.at[head * halves + b, seq * classes + c])
                for c in range(classes)
                for b in range(halves)
            ]
            _, total, out = functools.reduce(merge, slots)
            read_ref[seq, pl.ds(head * group, group), :] = out / total
    wait_bytes(other_gates, gate_send_sem)
    wait_bytes(plane, stage_send_sem.at[0])
    wait_bytes(along, stage_send_sem.at[1])
    wait_bytes(along, stage_send_sem.at[2])
    wait_bytes(plane, stage_send_sem.at[3])
    wait_bytes(cache_ref.at[pl.ds(0, piece), :], own_sem)
    sent = cache_ref.at[pl.ds(0, (devices - 1) * piece), :]
    wait_bytes(sent, send_sem)
    wait_bytes(sent, recv_sem)


def settle(cache_in, read_in, cache_out, read_out, sems):
    copies = [
        pltpu.make_async_copy(cache_in, cache_out, sems.at[0]),
        pltpu.make_async_copy(read_in, read_out, sems.at[1]),
    ]
    for copy in copies:
        copy.start()
    for copy in copies:
        copy.wait()


def solution(mesh):
    sp_count, tp_count = mesh.shape["sp"], mesh.shape["tp"]
    devices = sp_count * tp_count

    def shards(tokens, norm_gain, w_key, w_value, new_query, cum_gate):
        seqs, positions, width = tokens.shape
        heads = w_key.shape[1] // HD
        columns = w_key.shape[1]
        query_heads = new_query.shape[1]
        group = query_heads // heads
        length = cum_gate.shape[-1]
        tile = min(TILE, positions)
        part = (group // 2 + 1) * 2 * HD
        sizes = (sp_count, tp_count, seqs, heads, positions, width)
        vmem = pl.BlockSpec(memory_space=pltpu.VMEM)
        anywhere = pl.BlockSpec(memory_space=pltpu.HBM)
        cache, first_read = pl.pallas_call(
            functools.partial(kernel, sizes),
            out_shape=(
                pltpu.VMEM((length, 2 * HD), jnp.bfloat16),
                pltpu.VMEM((seqs, query_heads, HD), jnp.float32),
            ),
            in_specs=[anywhere] * 6,
            out_specs=(vmem, vmem),
            scratch_shapes=[
                pltpu.VMEM((seqs * positions // tile, tile, width), jnp.bfloat16),
                pltpu.VMEM((width, columns), jnp.bfloat16),
                pltpu.VMEM((width, columns), jnp.bfloat16),
                pltpu.VMEM((1, width), jnp.float32),
                pltpu.VMEM((seqs, heads, group, HD), jnp.bfloat16),
                pltpu.VMEM((1, length), jnp.float32),
                pltpu.VMEM((tile, width), jnp.bfloat16),
                pltpu.VMEM((seqs * heads, positions, 2 * HD), jnp.bfloat16),
                pltpu.VMEM((devices, 1, max(length // devices, 128)), jnp.float32),
                pltpu.VMEM((tp_count, sp_count, 1, part), jnp.float32),
                pltpu.VMEM((tp_count, sp_count, 1, part), jnp.float32),
                pltpu.VMEM((sp_count, 1, part), jnp.float32),
                pltpu.VMEM((sp_count, 1, part), jnp.float32),
                pltpu.VMEM((tp_count, sp_count, 1, part), jnp.float32),
                pltpu.SemaphoreType.DMA((seqs * positions // tile,)),
                pltpu.SemaphoreType.DMA((2,)),
                pltpu.SemaphoreType.DMA((5,)),
                *[pltpu.SemaphoreType.DMA] * 4,
                pltpu.SemaphoreType.DMA((4,)),
                pltpu.SemaphoreType.DMA((4,)),
                pltpu.SemaphoreType.DMA,
                pltpu.SemaphoreType.REGULAR,
            ],
            compiler_params=pltpu.CompilerParams(
                collective_id=0, has_side_effects=True, vmem_limit_bytes=VMEM_BYTES
            ),
        )(
            tokens,
            norm_gain.reshape(1, width),
            w_key,
            w_value,
            new_query.reshape(seqs, heads, group, HD),
            cum_gate.reshape(1, length),
        )
        cache, first_read = pl.pallas_call(
            settle,
            out_shape=(
                jax.ShapeDtypeStruct(cache.shape, cache.dtype),
                jax.ShapeDtypeStruct(first_read.shape, first_read.dtype),
            ),
            in_specs=[vmem] * 2,
            out_specs=(anywhere, anywhere),
            scratch_shapes=[pltpu.SemaphoreType.DMA((2,))],
            compiler_params=pltpu.CompilerParams(vmem_limit_bytes=VMEM_BYTES),
        )(
            pltpu.with_memory_space_constraint(cache, pltpu.VMEM),
            pltpu.with_memory_space_constraint(first_read, pltpu.VMEM),
        )
        return cache.reshape(1, 1, length, 2 * HD), first_read

    in_specs = (
        P("gr", ("sp", "tp"), None),
        P(),
        P(),
        P(),
        P("gr", None, None),
        P(("gr", "sp"), "tp", None),
    )
    out_specs = (P(("gr", "sp"), "tp", None, None), P("gr", None, None))
    return jax.shard_map(shards, mesh=mesh, in_specs=in_specs, out_specs=out_specs, check_vma=False)
```
